32 devices in a mesh: rep: 2 (over x), fs: 8 (over z, y), tp: 2 (over core).
Axes of the slice: x: 2, y: 2, z: 4, core: 2. Of those that a mesh axis runs over, the one named last changes fastest.
Arguments:
- inputs: bfloat16 [4096, 2048], P(('rep', 'fs', 'tp')), may hold values from -6 to 6
- cotangent: bfloat16 [4096, 2048], P(('rep', 'fs', 'tp')), may hold values from -6 to 6
- up_weight: bfloat16 [2048, 4096], P('fs', 'tp'), may hold values from -0.125 to 0.125
- down_weight: bfloat16 [4096, 2048], P('tp', 'fs'), may hold values from -0.09375 to 0.09375
Outputs:
- input_grad: bfloat16 [4096, 2048], P(('rep', 'fs', 'tp'))
- up_grad: float32 [2048, 4096], P('fs', 'tp')
- down_grad: float32 [4096, 2048], P('tp', 'fs')
The draws below stay inside these ranges and needn't reach their ends.
All inputs are finite; a program needn't handle non-finite values.
Results may differ from the reference program's by a relative error of at most 0.013.
Values may be sent and summed in bfloat16 or wider, within the bound.
A program may use at most 128 MiB of HBM per device.

```python
import jax
import jax.numpy as jnp
from jax import lax

D = 2048
FF = 4096
TOKENS = 4096
N_TP = 2


def raised(array, stream_key, source, target, blocks, factor):
    owner, partner = [(jnp.arange(array.shape[dim]) // (array.shape[dim] // blocks)).reshape([-1 if axis == dim else 1 for axis in range(array.ndim)]) for dim in (source, target)]
    chosen = jax.random.permutation(stream_key, blocks)[partner]
    strong = (owner == chosen) | (owner == (partner + blocks // 2) % blocks)
    return jnp.where(strong, factor * array, array)


def shard_levels(key, shape, pieces, low, top_value):
    def one(axis_at, blocks):
        steps = jax.random.uniform(jax.random.fold_in(jax.random.fold_in(key, 6), axis_at), (blocks,), jnp.float32, low / len(pieces), top_value / len(pieces))
        return jnp.repeat(jnp.exp(steps), shape[axis_at] // blocks).reshape((-1,) + (1,) * (len(shape) - axis_at - 1))

    level = one(*pieces[0])
    for cut in pieces[1:]:
        level = level * one(*cut)
    return level


def gaussian(key, shape, scale, bound, cuts=(), held_as=jnp.bfloat16):
    level = shard_levels(key, shape, cuts, -0.22, 0.18) if cuts else 1.0
    drawn = jax.random.normal(key, shape, jnp.float32) * scale * level
    return jnp.minimum(jnp.maximum(drawn, -bound), bound).astype(held_as)


def noise_with(stream_key, dims, deviation, bound, pieces, heavy, held_as=jnp.bfloat16):
    entries = deviation * jax.random.normal(stream_key, dims, jnp.float32)
    if pieces:
        entries = entries * shard_levels(stream_key, dims, pieces, -0.22, 0.18)
    return jnp.clip(raised(entries, jax.random.fold_in(stream_key, 3), *heavy), -bound, bound).astype(held_as)


def setup_inputs(seed: int = 0) -> dict:
    key_list = jax.random.split(jax.random.key(seed), 5)
    inputs = noise_with(key_list[0], (TOKENS, D), 1.0, 6.0, ((0, 32),), (0, 1, 32, 2.75))
    cotangent = noise_with(key_list[1], (TOKENS, D), 1.0, 6.0, ((0, 32),), (0, 1, 32, 2.75))
    up_weight = gaussian(key_list[2], (D, FF), D ** -0.5, 0.125, ((0, 8), (1, 2)))
    down_weight = gaussian(key_list[3], (FF, D), FF ** -0.5, 0.09375, ((0, 2), (1, 8)))
    return dict(inputs=inputs, cotangent=cotangent, up_weight=up_weight, down_weight=down_weight)


def reference(inputs, cotangent, up_weight, down_weight):
    pre_active = jnp.dot(inputs, up_weight, preferred_element_type=jnp.float32)
    active = jnp.maximum(pre_active, 0.0)
    activation = (active * active).astype(jnp.bfloat16)
    activation_grad = jnp.dot(cotangent, down_weight.T, preferred_element_type=jnp.float32)
    pre_grad = (2.0 * active * activation_grad).astype(jnp.bfloat16)
    block_width = FF // N_TP

    def add_block(index, running):
        offset = (index * block_width).astype(jnp.int32)
        grad_cols = lax.dynamic_slice_in_dim(pre_grad, offset, block_width, 1)
        weight_cols = lax.dynamic_slice_in_dim(up_weight, offset, block_width, 1)
        partial_sum = jnp.dot(grad_cols, weight_cols.T, preferred_element_type=jnp.float32)
        rounded = lax.optimization_barrier(partial_sum.astype(jnp.bfloat16))
        return running + rounded.astype(jnp.float32)

    start_sum = jnp.zeros((inputs.shape[0], D), jnp.float32)
    input_grad = lax.fori_loop(jnp.int32(0), jnp.int32(N_TP), add_block, start_sum).astype(jnp.bfloat16)
    loss_scale = TOKENS ** -0.5
    up_grad = jnp.dot(inputs.T, pre_grad, preferred_element_type=jnp.float32) * loss_scale
    down_grad = jnp.dot(activation.T, cotangent, preferred_element_type=jnp.float32) * loss_scale
    return (input_grad, up_grad, down_grad)
```

```python
import functools
import math

import jax
import jax.numpy as jnp
from jax import lax
from jax.experimental import pallas as pl
from jax.experimental.pallas import tpu as pltpu
from jax.sharding import PartitionSpec as P

MESH = pl.DeviceIdType.MESH
BF16, F32 = jnp.bfloat16, jnp.float32
NT = (((1,), (1,)), ((), ()))


def ring_place(f, n):
    odd = lax.rem(f, 2)
    half = lax.div(f, 2)
    return half * (1 - odd) + (n - 1 - half) * odd


def ring_member(p, n):
    back = lax.div(p, (n + 1) // 2)
    return 2 * p * (1 - back) + (2 * n - 1 - 2 * p) * back


def tile_of(size, most):
    while size % most:
        most //= 2
    return most


def kernel(
    R, n, T,
    x_ref, c_ref, u_ref, d_ref,
    ig_ref, gu_ref, gd_ref,
    xg, cg, xt, ug, dg, pre, agr, pg, at,
    igp, itr, isum, irr, us, ur, ds_, dr_, fu, fd, fur, fdr,
    ag_ss, ag_rs, rs_ss, rs_rs, tr_ss, tr_rs, tt_ss, tt_rs,
    it_ss, it_rs, ir_ss, ir_rs, f_ss, f_rs,
):
    r, f, t = lax.axis_index("rep"), lax.axis_index("fs"), lax.axis_index("tp")
    tok, db = x_ref.shape[1], x_ref.shape[2]
    hb = u_ref.shape[1]
    rows = R * T * tok
    p = ring_place(f, n)

    def member(q):
        return ring_member(lax.rem(p + q + n, n), n)

    def ring_dev(sign):
        return (r, member(sign), t)

    def rep_dev(q):
        return (lax.rem(r + q + R, R), f, t)

    def tp_dev(q):
        return (r, f, lax.rem(t + q + T, T))

    barrier = pltpu.get_barrier_semaphore()
    peers = [ring_dev(1), ring_dev(-1)]
    peers += [rep_dev(q) for q in range(1, R)] + [tp_dev(q) for q in range(1, T)]
    for peer in peers:
        pl.semaphore_signal(barrier, inc=1, device_id=peer, device_id_type=MESH)
    pl.semaphore_wait(barrier, len(peers))

    def remote(src, dst, ssem, rsem, dev):
        return pltpu.make_async_remote_copy(
            src_ref=src, dst_ref=dst, send_sem=ssem, recv_sem=rsem,
            device_id=dev, device_id_type=MESH,
        )

    long, short = n // 2, (n - 1) // 2
    streams = [(0, 1, long), (0, -1, short), (1, 1, short), (1, -1, long)]
    hops = max(long, short)
    own = (u_ref, d_ref)
    held = (ug, dg)

    def slot(sign, s):
        return (n - s if sign > 0 else s) - 1

    def gather_copy(i, s):
        g, sign, _ = streams[i]
        src = own[g] if s == 1 else held[g].at[slot(sign, s - 1)]
        return remote(
            src, held[g].at[slot(sign, s)], ag_ss.at[i, s - 1], ag_rs.at[i, s - 1],
            ring_dev(sign),
        )

    sends = []

    def go(copy):
        copy.start()
        sends.append(copy)
        return copy

    flying = {}
    for i, (g, sign, k) in enumerate(streams):
        if k >= 1:
            flying[i, 1] = go(gather_copy(i, 1))

    tokens = ((x_ref, xg), (c_ref, cg))

    def span(dt, dr):
        return pl.ds((dt * R + dr) * tok, tok)

    rep_copies = {}
    for dr in range(1, R):
        for j, (ref, full) in enumerate(tokens):
            rep_copies[j, dr] = go(remote(
                ref, full.at[:, span(0, dr), :], tr_ss.at[j, dr], tr_rs.at[j, dr], rep_dev(-dr)
            ))
    tp_copies = {}
    for dt in range(1, T):
        for j, (ref, full) in enumerate(tokens):
            tp_copies[j, dt, 0] = go(remote(
                ref, full.at[:, span(dt, 0), :], tt_ss.at[j, dt, 0], tt_rs.at[j, dt, 0],
                tp_dev(-dt),
            ))
    for ref, full in tokens:
        full[:, 0:tok, :] = ref[...]

    row_tile = tile_of(rows, 256)

    def gather_dot(g, block, q, first=False):
        b = member(q)
        out, full = ((pre, xg), (agr, cg))[g]

        @pl.loop(0, rows // row_tile)
        def _(i):
            part = pl.ds(pl.multiple_of(i * row_tile, row_tile), row_tile)
            lhs = full[b, part, :]
            if g == 0:
                val = jnp.dot(lhs, block[...], preferred_element_type=F32)
            else:
                val = lax.dot_general(lhs, block[...], NT, preferred_element_type=F32)
            if first:
                out[part, :] = val
            else:
                out[part, :] += val

    def finish_tokens():
        for dr in range(1, R):
            for j, (ref, full) in enumerate(tokens):
                rep_copies[j, dr].wait_recv()
                for dt in range(1, T):
                    tp_copies[j, dt, dr] = go(remote(
                        full.at[:, span(0, dr), :], full.at[:, span(dt, dr), :],
                        tt_ss.at[j, dt, dr], tt_rs.at[j, dt, dr], tp_dev(-dt),
                    ))
        for copy in tp_copies.values():
            copy.wait_recv()

        @pl.loop(0, n)
        def _(b):
            xt[b] = xg[b].T

        gather_dot(0, u_ref, 0, True)
        gather_dot(1, d_ref, 0, True)

    for s in range(1, hops + 1):
        for i, (g, sign, k) in enumerate(streams):
            if s <= k:
                flying[i, s].wait_recv()
                if s < k:
                    flying[i, s + 1] = go(gather_copy(i, s + 1))
        if s == 1:
            finish_tokens()
        for i, (g, sign, k) in enumerate(streams):
            if s <= k:
                gather_dot(g, held[g].at[slot(sign, s)], -sign * s)

    act_tile = tile_of(rows, 128)

    @pl.loop(0, rows // act_tile)
    def _(i):
        part = pl.ds(pl.multiple_of(i * act_tile, act_tile), act_tile)
        active = jnp.maximum(pre[part, :], 0.0)
        pg[part, :] = (2.0 * active * agr[part, :]).astype(BF16)
        at[:, part] = (active * active).astype(BF16).T

    def grad_block(g, q, dst, arrived):
        b = member(q)
        height = (db, hb)[g]
        tile = tile_of(height, 256)

        @pl.loop(0, height // tile)
        def _(i):
            part = pl.ds(pl.multiple_of(i * tile, tile), tile)
            if g == 0:
                val = jnp.dot(xt[b, part, :], pg[...], preferred_element_type=F32)
            else:
                val = jnp.dot(at[part, :], cg[b], preferred_element_type=F32)
            for a in arrived:
                val = val + a[part, :].astype(F32)
            dst[part, :] = val.astype(BF16)

    rs_send, rs_recv = (us, ds_), (ur, dr_)

    def rs_index(i, s):
        g, sign, _ = streams[i]
        return s - 1 if sign > 0 else (long, short)[g] + s - 1

    reducing = {}

    def reduce_step(i, s):
        g, sign, k = streams[i]
        arrived = []
        if s > 1:
            reducing[i, s - 1].wait_recv()
            arrived = [rs_recv[g].at[rs_index(i, s - 1)]]
        mine = rs_send[g].at[rs_index(i, s)]
        grad_block(g, sign * (k - s + 1), mine, arrived)
        reducing[i, s] = go(remote(
            mine, rs_recv[g].at[rs_index(i, s)], rs_ss.at[i, s - 1], rs_rs.at[i, s - 1],
            ring_dev(sign),
        ))

    for i, (g, sign, k) in enumerate(streams):
        if k >= 1:
            reduce_step(i, 1)

    for q in range(n):
        block = u_ref if q == 0 else ug.at[q - 1]
        b = member(q)

        @pl.loop(0, rows // row_tile)
        def _(i):
            part = pl.ds(pl.multiple_of(i * row_tile, row_tile), row_tile)
            igp[b, part, :] = lax.dot_general(
                pg[part, :], block[...], NT, preferred_element_type=F32
            ).astype(BF16)

    wide = R * tok
    it_copies = [
        go(remote(
            igp.at[:, pl.ds(dt * wide, wide), :], itr.at[dt - 1],
            it_ss.at[dt], it_rs.at[dt], tp_dev(dt),
        ))
        for dt in range(1, T)
    ]
    ir_copies = []

    def finish_tp():
        for copy in it_copies:
            copy.wait_recv()

        @pl.loop(0, n)
        def _(b):
            for dr in range(R):
                part = pl.ds(dr * tok, tok)
                val = igp[b, part, :].astype(F32)
                for dt in range(1, T):
                    val = val + itr[dt - 1, b, part, :].astype(F32)
                isum[dr, b] = val.astype(BF16)

        for dr in range(1, R):
            ir_copies.append(go(remote(
                isum.at[dr], irr.at[dr - 1], ir_ss.at[dr], ir_rs.at[dr], rep_dev(dr)
            )))

    def finish_rep():
        for copy in ir_copies:
            copy.wait_recv()

        @pl.loop(0, n)
        def _(b):
            val = isum[0, b].astype(F32)
            for dr in range(1, R):
                val = val + irr[dr - 1, b].astype(F32)
            ig_ref[b] = val.astype(BF16)

    finish_tp()
    for s in range(2, hops + 1):
        for i, (g, sign, k) in enumerate(streams):
            if s <= k:
                reduce_step(i, s)
        if s == 2:
            finish_rep()
    if hops < 2:
        finish_rep()

    finals = ((fu, fur, gu_ref), (fd, fdr, gd_ref))
    fin_copies = {}
    for g, (mine, theirs, out) in enumerate(finals):
        arrived = []
        for i, (h, sign, k) in enumerate(streams):
            if h == g and k >= 1:
                reducing[i, k].wait_recv()
                arrived.append(rs_recv[g].at[rs_index(i, k)])
        grad_block(g, 0, mine, arrived)
        for dr in range(1, R):
            fin_copies[g, dr] = go(remote(
                mine, theirs.at[dr - 1], f_ss.at[g, dr], f_rs.at[g, dr], rep_dev(-dr)
            ))
    for g, (mine, theirs, out) in enumerate(finals):
        out[r] = mine[...]
    for g, (mine, theirs, out) in enumerate(finals):
        for dr in range(1, R):
            fin_copies[g, dr].wait_recv()
            out[lax.rem(r + dr, R)] = theirs[dr - 1]
    for copy in sends:
        copy.wait_send()


def shards(inputs, cotangent, up_weight, down_weight):
    R, n, T = lax.axis_size("rep"), lax.axis_size("fs"), lax.axis_size("tp")
    tok, D = inputs.shape
    db, hb = up_weight.shape[0], up_weight.shape[1] // R
    rows = R * T * tok
    r = lax.axis_index("rep")
    by_block = lambda a: a.reshape(tok, n, db).swapaxes(0, 1)
    up = lax.dynamic_slice_in_dim(up_weight, r * hb, hb, 1)
    down = lax.dynamic_slice_in_dim(down_weight, r * hb, hb, 0)
    V, S = pltpu.VMEM, pltpu.SemaphoreType.DMA
    hops = max(n // 2, 1)
    m = max(n - 1, 1)
    scratch = [
        V((n, rows, db), BF16), V((n, rows, db), BF16), V((n, db, rows), BF16),
        V((m, db, hb), BF16), V((m, hb, db), BF16),
        V((rows, hb), F32), V((rows, hb), F32), V((rows, hb), BF16), V((hb, rows), BF16),
        V((n, rows, db), BF16), V((max(T - 1, 1), n, R * tok, db), BF16),
        V((R, n, tok, db), BF16), V((max(R - 1, 1), n, tok, db), BF16),
        V((m, db, hb), BF16), V((m, db, hb), BF16), V((m, hb, db), BF16), V((m, hb, db), BF16),
        V((db, hb), BF16), V((hb, db), BF16),
        V((max(R - 1, 1), db, hb), BF16), V((max(R - 1, 1), hb, db), BF16),
        S((4, hops)), S((4, hops)), S((4, hops)), S((4, hops)),
        S((2, R)), S((2, R)), S((2, T, R)), S((2, T, R)),
        S((T,)), S((T,)), S((R,)), S((R,)), S((2, R)), S((2, R)),
    ]
    vmem = pl.BlockSpec(memory_space=pltpu.VMEM)
    ig, gu, gd = pl.pallas_call(
        functools.partial(kernel, R, n, T),
        out_shape=(
            jax.ShapeDtypeStruct((n, tok, db), BF16),
            jax.ShapeDtypeStruct((R, db, hb), BF16),
            jax.ShapeDtypeStruct((R, hb, db), BF16),
        ),
        in_specs=[vmem] * 4,
        out_specs=(vmem,) * 3,
        scratch_shapes=scratch,
        compiler_params=pltpu.CompilerParams(
            collective_id=0, has_side_effects=True, vmem_limit_bytes=60 * 2**20
        ),
    )(by_block(inputs), by_block(cotangent), up, down)
    total_tokens = tok * R * n * T
    loss_scale = 1.0 / math.sqrt(total_tokens)
    input_grad = ig.swapaxes(0, 1).reshape(tok, D)
    up_grad = gu.swapaxes(0, 1).reshape(db, R * hb).astype(F32) * loss_scale
    down_grad = gd.reshape(R * hb, db).astype(F32) * loss_scale
    return input_grad, up_grad, down_grad


def solution(mesh):
    token, up, down = P(("rep", "fs", "tp"), None), P("fs", "tp"), P("tp", "fs")
    return jax.shard_map(
        shards,
        mesh=mesh,
        in_specs=(token, token, up, down),
        out_specs=(token, up, down),
        check_vma=False,
    )
```

```python
import functools
import math

import jax
import jax.numpy as jnp
from jax import lax
from jax.experimental import pallas as pl
from jax.experimental.pallas import tpu as pltpu
from jax.sharding import PartitionSpec as P

MESH = pl.DeviceIdType.MESH
CHUNKS = 2
BF16, F32 = jnp.bfloat16, jnp.float32
NT = (((1,), (1,)), ((), ()))


def ring_place(f, n):
    odd = lax.rem(f, 2)
    half = lax.div(f, 2)
    return half * (1 - odd) + (n - 1 - half) * odd


def ring_member(p, n):
    back = lax.div(p, (n + 1) // 2)
    return 2 * p * (1 - back) + (2 * n - 1 - 2 * p) * back


def tile_of(size, most):
    while size % most:
        most //= 2
    return most


def kernel(
    R, n, T,
    x_ref, c_ref, u_ref, d_ref,
    ig_ref, gu_ref, gd_ref,
    xg, cg, xt, ug, dg, pre, agr, pg, at,
    igp, itr, isum, irr, us, ur, ds_, dr_, fu, fd, fur, fdr,
    ag_ss, ag_rs, rs_ss, rs_rs, tr_ss, tr_rs, tt_ss, tt_rs,
    it_ss, it_rs, ir_ss, ir_rs, f_ss, f_rs,
):
    r, f, t = lax.axis_index("rep"), lax.axis_index("fs"), lax.axis_index("tp")
    tok, db = x_ref.shape[0], u_ref.shape[0]
    C, w = pre.shape[0], pre.shape[2]
    hb = C * w
    rows = R * T * tok

    def hidden(place, ch):
        return pl.ds(pl.multiple_of(place * hb + ch * w, w), w)

    for ref, full in ((x_ref, xg), (c_ref, cg)):
        for q in range(n):
            full[q, 0:tok, :] = ref[:, q * db:(q + 1) * db]
    p = ring_place(f, n)

    def member(q):
        return ring_member(lax.rem(p + q + n, n), n)

    def ring_dev(sign):
        return (r, member(sign), t)

    def rep_dev(q):
        return (lax.rem(r + q + R, R), f, t)

    def tp_dev(q):
        return (r, f, lax.rem(t + q + T, T))

    barrier = pltpu.get_barrier_semaphore()
    peers = [ring_dev(1), ring_dev(-1)]
    peers += [rep_dev(q) for q in range(1, R)] + [tp_dev(q) for q in range(1, T)]
    for peer in peers:
        pl.semaphore_signal(barrier, inc=1, device_id=peer, device_id_type=MESH)
    pl.semaphore_wait(barrier, len(peers))

    def remote(src, dst, ssem, rsem, dev):
        return pltpu.make_async_remote_copy(
            src_ref=src, dst_ref=dst, send_sem=ssem, recv_sem=rsem,
            device_id=dev, device_id_type=MESH,
        )

    long, short = n // 2, (n - 1) // 2
    streams = [(0, 1, long), (0, -1, short), (1, 1, short), (1, -1, long)]
    hops = max(long, short)
    def own(g, ch):
        return u_ref.at[:, hidden(r, ch)] if g == 0 else d_ref.at[hidden(r, ch), :]

    held = (ug, dg)

    def slot(sign, s):
        return (n - s if sign > 0 else s) - 1

    def gather_copy(ch, i, s):
        g, sign, _ = streams[i]
        src = own(g, ch) if s == 1 else held[g].at[slot(sign, s - 1), ch]
        return remote(
            src, held[g].at[slot(sign, s), ch],
            ag_ss.at[ch, i, s - 1], ag_rs.at[ch, i, s - 1], ring_dev(sign),
        )

    sends = []

    def go(copy):
        copy.start()
        sends.append(copy)
        return copy

    flying = {}

    def gather_first(ch):
        for i, (g, sign, k) in enumerate(streams):
            if k >= 1:
                flying[ch, i, 1] = go(gather_copy(ch, i, 1))

    gather_first(0)

    tokens = tuple((full.at[:, 0:tok, :], full) for full in (xg, cg))

    def span(dt, dr):
        return pl.ds((dt * R + dr) * tok, tok)

    rep_copies = {}
    for dr in range(1, R):
        for j, (ref, full) in enumerate(tokens):
            rep_copies[j, dr] = go(remote(
                ref, full.at[:, span(0, dr), :], tr_ss.at[j, dr], tr_rs.at[j, dr], rep_dev(-dr)
            ))
    tp_copies = {}
    for dt in range(1, T):
        for j, (ref, full) in enumerate(tokens):
            tp_copies[j, dt, 0] = go(remote(
                ref, full.at[:, span(dt, 0), :], tt_ss.at[j, dt, 0], tt_rs.at[j, dt, 0],
                tp_dev(-dt),
            ))

    row_tile = tile_of(rows, 256)

    def gather_dot(ch, g, block, q, first=False):
        b = member(q)
        out, full = ((pre, xg), (agr, cg))[g]

        @pl.loop(0, rows // row_tile)
        def _(i):
            part = pl.ds(pl.multiple_of(i * row_tile, row_tile), row_tile)
            lhs = full[b, part, :]
            if g == 0:
                val = jnp.dot(lhs, block[...], preferred_element_type=F32)
            else:
                val = lax.dot_general(lhs, block[...], NT, preferred_element_type=F32)
            if first:
                out[ch, part, :] = val
            else:
                out[ch, part, :] += val

    def finish_tokens():
        for dr in range(1, R):
            for j, (ref, full) in enumerate(tokens):
                rep_copies[j, dr].wait_recv()
                for dt in range(1, T):
                    tp_copies[j, dt, dr] = go(remote(
                        full.at[:, span(0, dr), :], full.at[:, span(dt, dr), :],
                        tt_ss.at[j, dt, dr], tt_rs.at[j, dt, dr], tp_dev(-dt),
                    ))
        for copy in tp_copies.values():
            copy.wait_recv()

        @pl.loop(0, n)
        def _(b):
            xt[b] = xg[b].T

        for ch in range(C):
            gather_dot(ch, 0, own(0, ch), 0, True)
            gather_dot(ch, 1, own(1, ch), 0, True)

    act_tile = tile_of(rows, 128)

    def activate(ch):
        @pl.loop(0, rows // act_tile)
        def _(i):
            part = pl.ds(pl.multiple_of(i * act_tile, act_tile), act_tile)
            active = jnp.maximum(pre[ch, part, :], 0.0)
            pg[ch, part, :] = (2.0 * active * agr[ch, part, :]).astype(BF16)
            at[ch, :, part] = (active * active).astype(BF16).T

    def gather(ch, before_last):
        for s in range(1, hops + 1):
            if s == hops:
                before_last()
            for i, (g, sign, k) in enumerate(streams):
                if s <= k:
                    flying[ch, i, s].wait_recv()
                    if s < k:
                        flying[ch, i, s + 1] = go(gather_copy(ch, i, s + 1))
            if s == 1 and ch == 0:
                finish_tokens()
            for i, (g, sign, k) in enumerate(streams):
                if s <= k:
                    gather_dot(ch, g, held[g].at[slot(sign, s), ch], -sign * s)
        if hops == 0:
            if ch == 0:
                finish_tokens()
            before_last()
        activate(ch)

    def grad_block(ch, g, q, dst, arrived):
        b = member(q)
        height = (db, w)[g]
        tile = tile_of(height, 256)

        @pl.loop(0, height // tile)
        def _(i):
            part = pl.ds(pl.multiple_of(i * tile, tile), tile)
            if g == 0:
                val = jnp.dot(xt[b, part, :], pg[ch], preferred_element_type=F32)
            else:
                val = jnp.dot(at[ch, part, :], cg[b], preferred_element_type=F32)
            for a in arrived:
                val = val + a[part, :].astype(F32)
            dst[part, :] = val.astype(BF16)

    rs_send, rs_recv = (us, ds_), (ur, dr_)

    def rs_index(i, s):
        g, sign, _ = streams[i]
        return s - 1 if sign > 0 else (long, short)[g] + s - 1

    reducing = {}

    def reduce_step(ch, i, s):
        g, sign, k = streams[i]
        arrived = []
        if s > 1:
            reducing[ch, i, s - 1].wait_recv()
            arrived = [rs_recv[g].at[rs_index(i, s - 1), ch]]
        mine = rs_send[g].at[rs_index(i, s), ch]
        grad_block(ch, g, sign * (k - s + 1), mine, arrived)
        reducing[ch, i, s] = go(remote(
            mine, rs_recv[g].at[rs_index(i, s), ch],
            rs_ss.at[ch, i, s - 1], rs_rs.at[ch, i, s - 1], ring_dev(sign),
        ))

    def reduce_all(ch, s):
        for i, (g, sign, k) in enumerate(streams):
            if s <= k:
                reduce_step(ch, i, s)

    for ch in range(C):
        if ch + 1 < C:
            gather(ch, functools.partial(gather_first, ch + 1))
        elif C > 1:
            gather(ch, functools.partial(reduce_all, 0, 1))
        else:
            gather(ch, lambda: None)
            reduce_all(ch, 1)

    for q in range(n):
        b = member(q)

        @pl.loop(0, rows // row_tile)
        def _(i):
            part = pl.ds(pl.multiple_of(i * row_tile, row_tile), row_tile)
            val = 0.0
            for ch in range(C):
                block = own(0, ch) if q == 0 else ug.at[q - 1, ch]
                val = val + lax.dot_general(
                    pg[ch, part, :], block[...], NT, preferred_element_type=F32
                )
            igp[b, part, :] = val.astype(BF16)

    wide = R * tok
    it_copies = [
        go(remote(
            igp.at[:, pl.ds(dt * wide, wide), :], itr.at[dt - 1],
            it_ss.at[dt], it_rs.at[dt], tp_dev(dt),
        ))
        for dt in range(1, T)
    ]
    ir_copies = []

    def finish_tp():
        for copy in it_copies:
            copy.wait_recv()

        @pl.loop(0, n)
        def _(b):
            for dr in range(R):
                part = pl.ds(dr * tok, tok)
                val = igp[b, part, :].astype(F32)
                for dt in range(1, T):
                    val = val + itr[dt - 1, b, part, :].astype(F32)
                isum[dr, b] = val.astype(BF16)

        for dr in range(1, R):
            ir_copies.append(go(remote(
                isum.at[dr], irr.at[dr - 1], ir_ss.at[dr], ir_rs.at[dr], rep_dev(dr)
            )))

    def finish_rep():
        for copy in ir_copies:
            copy.wait_recv()

        for b in range(n):
            val = isum[0, b].astype(F32)
            for dr in range(1, R):
                val = val + irr[dr - 1, b].astype(F32)
            ig_ref[:, b * db:(b + 1) * db] = val.astype(BF16)

    finish_tp()

    finals = ((fu, fur, gu_ref), (fd, fdr, gd_ref))
    fin_copies = {}

    def put(g, place, ch, val):
        if g == 0:
            gu_ref[:, hidden(place, ch)] = val
        else:
            gd_ref[hidden(place, ch), :] = val

    def finish(ch, g):
        mine, theirs, out = finals[g]
        arrived = []
        for i, (h, sign, k) in enumerate(streams):
            if h == g and k >= 1:
                reducing[ch, i, k].wait_recv()
                arrived.append(rs_recv[g].at[rs_index(i, k), ch])
        grad_block(ch, g, 0, mine.at[ch], arrived)
        for dr in range(1, R):
            fin_copies[ch, g, dr] = go(remote(
                mine.at[ch], theirs.at[dr - 1, ch],
                f_ss.at[ch, g, dr], f_rs.at[ch, g, dr], rep_dev(-dr),
            ))
        put(g, r, ch, mine[ch])

    for ch in range(C):
        for s in range(2, hops + 1):
            reduce_all(ch, s)
            if ch == 0 and s == 2:
                finish_rep()
        if ch == 0 and hops < 2:
            finish_rep()
        if ch + 1 < C:
            reduce_all(ch + 1, 1)
        for g in range(2):
            finish(ch, g)
    for (ch, g, dr), copy in fin_copies.items():
        _, theirs, out = finals[g]
        copy.wait_recv()
        put(g, lax.rem(r + dr, R), ch, theirs[dr - 1, ch])
    for copy in sends:
        copy.wait_send()


def shards(inputs, cotangent, up_weight, down_weight):
    R, n, T = lax.axis_size("rep"), lax.axis_size("fs"), lax.axis_size("tp")
    tok, D = inputs.shape
    db, hb = up_weight.shape[0], up_weight.shape[1] // R
    rows = R * T * tok
    C = tile_of(hb // 128, CHUNKS) if hb > 128 else 1
    w = hb // C
    V, S = pltpu.VMEM, pltpu.SemaphoreType.DMA
    hops = max(n // 2, 1)
    m = max(n - 1, 1)
    scratch = [
        V((n, rows, db), BF16), V((n, rows, db), BF16), V((n, db, rows), BF16),
        V((m, C, db, w), BF16), V((m, C, w, db), BF16),
        V((C, rows, w), F32), V((C, rows, w), F32), V((C, rows, w), BF16), V((C, w, rows), BF16),
        V((n, rows, db), BF16), V((max(T - 1, 1), n, R * tok, db), BF16),
        V((R, n, tok, db), BF16), V((max(R - 1, 1), n, tok, db), BF16),
        V((m, C, db, w), BF16), V((m, C, db, w), BF16),
        V((m, C, w, db), BF16), V((m, C, w, db), BF16),
        V((C, db, w), BF16), V((C, w, db), BF16),
        V((max(R - 1, 1), C, db, w), BF16), V((max(R - 1, 1), C, w, db), BF16),
        S((C, 4, hops)), S((C, 4, hops)), S((C, 4, hops)), S((C, 4, hops)),
        S((2, R)), S((2, R)), S((2, T, R)), S((2, T, R)),
        S((T,)), S((T,)), S((R,)), S((R,)), S((C, 2, R)), S((C, 2, R)),
    ]
    vmem = pl.BlockSpec(memory_space=pltpu.VMEM)
    ig, gu, gd = pl.pallas_call(
        functools.partial(kernel, R, n, T),
        out_shape=(
            jax.ShapeDtypeStruct((tok, D), BF16),
            jax.ShapeDtypeStruct((db, R * hb), BF16),
            jax.ShapeDtypeStruct((R * hb, db), BF16),
        ),
        in_specs=[vmem] * 4,
        out_specs=(vmem,) * 3,
        scratch_shapes=scratch,
        compiler_params=pltpu.CompilerParams(
            collective_id=0, has_side_effects=True, vmem_limit_bytes=60 * 2**20
        ),
    )(inputs, cotangent, up_weight, down_weight)
    total_tokens = tok * R * n * T
    loss_scale = 1.0 / math.sqrt(total_tokens)
    return ig, gu.astype(F32) * loss_scale, gd.astype(F32) * loss_scale


def solution(mesh):
    token, up, down = P(("rep", "fs", "tp"), None), P("fs", "tp"), P("tp", "fs")
    return jax.shard_map(
        shards,
        mesh=mesh,
        in_specs=(token, token, up, down),
        out_specs=(token, up, down),
        check_vma=False,
    )
```
